512 devices in a mesh: fs: 64 (over z, y), tp: 8 (over x, core).
Axes of the slice: x: 4, y: 4, z: 16, core: 2. Of those that a mesh axis runs over, the one named last changes fastest.
Arguments:
- tokens: bfloat16 [49152, 2048], P('fs'), may hold values from -6 to 6
- norm_gain: float32 [2048], replicated, may hold values from 0.1 to 1.9
- gate_weight: float32 [2048, 5120], P('fs', 'tp'), may hold values from -0.125 to 0.125
- value_weight: float32 [2048, 5120], P('fs', 'tp'), may hold values from -0.125 to 0.125
- gate_scale: float32 [5120], P('tp'), may hold values from 0.3 to 3
- value_scale: float32 [5120], P('tp'), may hold values from 0.3 to 3
- gate_kernel: float32 [3, 5120], P(None, 'tp'), may hold values from -3.5 to 3.5
- value_kernel: float32 [3, 5120], P(None, 'tp'), may hold values from -3.5 to 3.5
- gate_bias: float32 [5120], P('tp'), may hold values from -3 to 3
- value_bias: float32 [5120], P('tp'), may hold values from -3 to 3
- down_weight: float32 [5120, 2048], P('tp', 'fs'), may hold values from -0.078125 to 0.078125
- down_scale: float32 [2048], P('tp'), may hold values from 0.3 to 3
Outputs:
- mixed: bfloat16 [49152, 2048], P('fs', 'tp')
The draws below stay inside these ranges and needn't reach their ends.
All inputs are finite; a program needn't handle non-finite values.
Results may differ from the reference program's by a relative error of at most 0.014.
Values may be sent and summed in bfloat16 or wider, within the bound.
No kernel may reach another device: no remote copies, remote signals or barrier semaphores. Data moves between devices by JAX's collectives and lax.ppermute only.
A program may use at most 64 MiB of HBM per device.

```python
import math
import jax
import jax.numpy as jnp
from jax import lax

D = 2048
FF = 5120
KERNEL = 3
TOK = 768
TOKENS = 49152
N_FS = 64
N_TP = 8


def block_scale(own_key, extent, shards, least, high):
    loudness, own = 1.0, jax.random.fold_in(own_key, 6)
    for dim, shards_of in shards:
        draws = jnp.exp(jax.random.uniform(jax.random.fold_in(own, dim), (shards_of,), jnp.float32, least / len(shards), high / len(shards)))
        loudness = loudness * jnp.repeat(draws, extent[dim] // shards_of).reshape([-1 if axis == dim else 1 for axis in range(len(extent))])
    return loudness


def gaussian(rng, extent, scale, most, cuts=(), held_as=jnp.bfloat16):
    level = block_scale(rng, extent, cuts, -0.22, 0.18) if cuts else 1.0
    entries = jax.random.normal(rng, extent, jnp.float32) * scale * level
    return jnp.minimum(jnp.maximum(entries, -most), most).astype(held_as)


def setup_inputs(seed: int = 0) -> dict:
    keys = jax.random.split(jax.random.key(seed), 13)
    return {
        "tokens": gaussian(keys[0], (TOKENS, D), 1.0, 6.0, ((0, 64),)),
        "norm_gain": jnp.clip(1.0 + 0.18 * jax.random.normal(keys[1], (D,), jnp.float32), 0.1, 1.9),
        "gate_weight": gaussian(keys[2], (D, FF), D ** -0.5, 0.125, ((0, 64), (1, 8)), jnp.float32),
        "value_weight": gaussian(keys[3], (D, FF), D ** -0.5, 0.125, ((0, 64), (1, 8)), jnp.float32),
        "gate_scale": jnp.clip(jnp.exp(math.log(3.0) - 2.3025851 * jax.random.uniform(keys[4], (FF,), jnp.float32) ** block_scale(keys[4], (FF,), ((0, 8),), -0.2, 0.2)), 0.3, 3.0),
        "value_scale": jnp.clip(jnp.exp(math.log(3.0) - 2.3025851 * jax.random.uniform(keys[5], (FF,), jnp.float32) ** block_scale(keys[5], (FF,), ((0, 8),), -0.2, 0.2)), 0.3, 3.0),
        "gate_kernel": gaussian(keys[6], (KERNEL, FF), KERNEL ** -0.5, 3.5, ((1, 8),), jnp.float32),
        "value_kernel": gaussian(keys[7], (KERNEL, FF), KERNEL ** -0.5, 3.5, ((1, 8),), jnp.float32),
        "gate_bias": gaussian(keys[8], (FF,), 0.5, 3.0, ((0, 8),), jnp.float32),
        "value_bias": gaussian(keys[9], (FF,), 0.5, 3.0, ((0, 8),), jnp.float32),
        "down_weight": gaussian(keys[10], (FF, D), FF ** -0.5, 0.078125, ((0, 8), (1, 64)), jnp.float32),
        "down_scale": jnp.clip(jnp.exp(math.log(3.0) - 2.3025851 * jax.random.uniform(keys[11], (D,), jnp.float32) ** block_scale(keys[11], (D,), ((0, 8),), -0.2, 0.2)), 0.3, 3.0),
    }


epsilon = 1e-06

def normalize(tokens, norm_gain):
    values = tokens.astype(jnp.float32)
    scaled = values * lax.rsqrt(lax.optimization_barrier(jnp.mean(values * values, axis=1, keepdims=True)) + epsilon)
    return (scaled * norm_gain[None, :]).astype(jnp.bfloat16)

def causal_mix(current, previous, kernel, tap_bias):
    row_count = current.shape[0]
    joined = jnp.concatenate([previous, current], axis=0).astype(jnp.float32)
    summed_taps = tap_bias[None, :] + kernel[2][None, :] * joined[2:]
    for back_by in (1, 2):
        summed_taps = summed_taps + kernel[2 - back_by][None, :] * joined[2 - back_by:2 - back_by + row_count]
    return summed_taps

def reference(tokens, norm_gain, gate_weight, value_weight, gate_scale, value_scale, gate_kernel, value_kernel, gate_bias, value_bias, down_weight, down_scale):
    gate_low = gate_weight.astype(jnp.bfloat16)
    value_low = value_weight.astype(jnp.bfloat16)
    down_low = down_weight.astype(jnp.bfloat16)
    block_width = FF // N_TP

    def one_block(carry, block_rows):
        previous_gate, previous_value = carry
        normed = normalize(block_rows, norm_gain)
        gate_pre = (jnp.dot(normed, gate_low, preferred_element_type=jnp.float32) * gate_scale[None, :]).astype(jnp.bfloat16)
        value_pre = (jnp.dot(normed, value_low, preferred_element_type=jnp.float32) * value_scale[None, :]).astype(jnp.bfloat16)
        gate_conv = causal_mix(gate_pre, previous_gate, gate_kernel, gate_bias)
        value_conv = causal_mix(value_pre, previous_value, value_kernel, value_bias)
        hidden = (jax.nn.gelu(gate_conv, approximate=True) * value_conv).astype(jnp.bfloat16)
        summed = jnp.zeros((block_rows.shape[0], D), jnp.float32)
        for block_index in range(N_TP):
            first_col = block_index * block_width
            partial_term = jnp.dot(hidden[:, first_col:first_col + block_width], down_low[first_col:first_col + block_width], preferred_element_type=jnp.float32).astype(jnp.bfloat16)
            partial_term = lax.optimization_barrier(partial_term)
            summed = summed + partial_term.astype(jnp.float32)
        result = (summed * down_scale[None, :]).astype(jnp.bfloat16)
        return ((gate_pre[-2:], value_pre[-2:]), result)
    start = (jnp.zeros((2, FF), jnp.bfloat16), jnp.zeros((2, FF), jnp.bfloat16))
    final_carry, mixed = lax.scan(one_block, start, tokens.reshape(N_FS, TOK, D))
    return mixed.reshape(TOKENS, D)
```

```python
import jax
import jax.numpy as jnp
from jax import lax
from jax.experimental import pallas as pl
from jax.experimental.pallas import tpu as pltpu
from jax.sharding import Mesh, PartitionSpec as P

epsilon = 1e-06
up_lift = 2.0**17
down_lift = 2.0**19
NT = (((1,), (1,)), ((), ()))


def first_half(which, hidden, rows, out):
    out[0] = lax.dot_general(
        hidden[...], rows[0, 0], NT, preferred_element_type=jnp.float32
    ).astype(jnp.bfloat16)


def second_half(which, hidden, rows, received, out):
    product = lax.dot_general(hidden[...], rows[0, 0], NT, preferred_element_type=jnp.float32)
    out[0] = (product + received[0].astype(jnp.float32)).astype(jnp.bfloat16)


def down_part(which, hidden, rows, received=None):
    groups, _, width, depth = rows.shape
    count = hidden.shape[0]
    block = pl.BlockSpec((1, count, width), lambda i, w: (i, 0, 0))
    in_specs = [
        pl.BlockSpec((count, depth), lambda i, w: (0, 0)),
        pl.BlockSpec((1, 1, width, depth), lambda i, w: (i, w[0], 0, 0)),
    ]
    operands = [hidden, rows]
    if received is not None:
        in_specs.append(block)
        operands.append(received)
    return pl.pallas_call(
        first_half if received is None else second_half,
        grid_spec=pltpu.PrefetchScalarGridSpec(
            num_scalar_prefetch=1, grid=(groups,), in_specs=in_specs, out_specs=block
        ),
        out_shape=jax.ShapeDtypeStruct((groups, count, width), jnp.bfloat16),
    )(which, *operands)


def causal_mix(current, previous, kernel, tap_bias):
    row_count = current.shape[0]
    joined = jnp.concatenate([previous, current], axis=0).astype(jnp.float32)
    summed_taps = tap_bias[None, :] + kernel[2][None, :] * joined[2:]
    for back_by in (1, 2):
        summed_taps = (
            summed_taps
            + kernel[2 - back_by][None, :] * joined[2 - back_by : 2 - back_by + row_count]
        )
    return summed_taps


def body(
    tokens,
    norm_gain,
    gate_weight,
    value_weight,
    gate_scale,
    value_scale,
    gate_kernel,
    value_kernel,
    gate_bias,
    value_bias,
    down_weight,
    down_scale,
):
    z_count, y_count = lax.axis_size("z"), lax.axis_size("y")
    x_count, c_count = lax.axis_size("x"), lax.axis_size("c")
    place = lax.axis_index("z") * y_count + lax.axis_index("y")
    core = lax.axis_index("c")
    row_count, width = tokens.shape
    piece, units = gate_weight.shape

    gain = lax.dynamic_slice(norm_gain, (place * piece,), (piece,))[:, None] * up_lift
    shard = jnp.concatenate(
        [gate_weight * gain, value_weight * gain, down_weight.T * down_lift], axis=1
    ).astype(jnp.float16)
    over_z = lax.all_gather(shard, "z", axis=0)
    full = lax.all_gather(over_z, "y", axis=1, tiled=True).reshape(width, 3 * units)

    values = tokens.astype(jnp.float32)
    factor = lax.rsqrt(jnp.mean(values * values, axis=1, keepdims=True) + epsilon) / up_lift
    pre = []
    for at, scale in ((0, gate_scale), (units, value_scale)):
        raw = jnp.dot(
            tokens,
            full[:, at : at + units].astype(jnp.bfloat16),
            preferred_element_type=jnp.float32,
        )
        pre.append((raw * (factor * scale[None, :])).astype(jnp.bfloat16))
    tails = jnp.concatenate([p[row_count - 2 :] for p in pre], axis=1)
    previous = lax.ppermute(
        tails,
        ("z", "y"),
        [(source, source + 1) for source in range(z_count * y_count - 1)],
    )
    gate_conv = causal_mix(pre[0], previous[:, :units], gate_kernel, gate_bias)
    value_conv = causal_mix(pre[1], previous[:, units:], value_kernel, value_bias)
    hidden = (jax.nn.gelu(gate_conv, approximate=True) * value_conv).astype(jnp.bfloat16)

    rows = full[:, 2 * units :].astype(jnp.bfloat16)
    rows = rows.reshape(x_count, c_count, width // (x_count * c_count), units)
    sent = down_part((1 - core).reshape(1), hidden, rows)
    received = lax.ppermute(sent, "c", [(0, 1), (1, 0)])
    paired = down_part(core.reshape(1), hidden, rows, received)
    parts = lax.all_to_all(paired, "x", 0, 0)
    summed = jnp.sum(parts.astype(jnp.float32), axis=0)
    return (summed * (down_scale / down_lift)[None, :]).astype(jnp.bfloat16)


def solution(mesh):
    grid = Mesh(mesh.devices.reshape(16, 4, 4, 2), ("z", "y", "x", "c"))
    fs, tp = ("z", "y"), ("x", "c")
    return jax.shard_map(
        body,
        mesh=grid,
        in_specs=(
            P(fs, None),
            P(),
            P(fs, tp),
            P(fs, tp),
            P(tp),
            P(tp),
            P(None, tp),
            P(None, tp),
            P(tp),
            P(tp),
            P(tp, fs),
            P(tp),
        ),
        out_specs=P(fs, tp),
        check_vma=False,
    )
```

```python
import jax
import jax.numpy as jnp
from jax import lax
from jax.experimental.layout import Layout, with_layout_constraint
from jax.sharding import Mesh, PartitionSpec as P

epsilon = 1e-06
up_lift = 2.0**17
down_lift = 2.0**19


def down_half(hidden, rows, core):
    groups, _, part, total = rows.shape
    units = hidden.shape[1]
    mine = lax.dynamic_slice(rows, (0, core, 0, total - units), (groups, 1, part, units))
    mine = mine.reshape(groups * part, units).astype(jnp.bfloat16)
    product = lax.dot_general(
        mine, hidden, (((1,), (1,)), ((), ())), preferred_element_type=jnp.float32
    )
    return product.reshape(groups, part, -1)


def causal_mix(current, previous, kernel, tap_bias):
    row_count = current.shape[0]
    joined = jnp.concatenate([previous, current], axis=0).astype(jnp.float32)
    summed_taps = tap_bias[None, :] + kernel[2][None, :] * joined[2:]
    for back_by in (1, 2):
        summed_taps = (
            summed_taps
            + kernel[2 - back_by][None, :] * joined[2 - back_by : 2 - back_by + row_count]
        )
    return summed_taps


def body(
    tokens,
    norm_gain,
    gate_weight,
    value_weight,
    gate_scale,
    value_scale,
    gate_kernel,
    value_kernel,
    gate_bias,
    value_bias,
    down_weight,
    down_scale,
):
    z_count, y_count = lax.axis_size("z"), lax.axis_size("y")
    x_count, c_count = lax.axis_size("x"), lax.axis_size("c")
    place = lax.axis_index("z") * y_count + lax.axis_index("y")
    core = lax.axis_index("c")
    row_count, width = tokens.shape
    piece, units = gate_weight.shape

    gain = lax.dynamic_slice(norm_gain, (place * piece,), (piece,))[:, None] * up_lift
    shard = jnp.concatenate(
        [gate_weight * gain, value_weight * gain, down_weight.T * down_lift], axis=1
    ).astype(jnp.float16)
    over_z = lax.all_gather(shard, "z", axis=0)
    full = lax.all_gather(over_z, "y", axis=1, tiled=True).reshape(width, 3 * units)
    tokens, full = lax.optimization_barrier((tokens, full))

    values = tokens.astype(jnp.float32)
    factor = lax.rsqrt(jnp.mean(values * values, axis=1, keepdims=True) + epsilon) / up_lift
    pre = []
    for at, scale in ((0, gate_scale), (units, value_scale)):
        raw = jnp.dot(
            tokens,
            full[:, at : at + units].astype(jnp.bfloat16),
            preferred_element_type=jnp.float32,
        )
        pre.append((raw * (factor * scale[None, :])).astype(jnp.bfloat16))
    tails = jnp.concatenate([p[row_count - 2 :] for p in pre], axis=1)
    previous = lax.ppermute(
        tails,
        ("z", "y"),
        [(source, source + 1) for source in range(z_count * y_count - 1)],
    )
    gate_conv = causal_mix(pre[0], previous[:, :units], gate_kernel, gate_bias)
    value_conv = causal_mix(pre[1], previous[:, units:], value_kernel, value_bias)
    hidden = (jax.nn.gelu(gate_conv, approximate=True) * value_conv).astype(jnp.bfloat16)
    hidden = with_layout_constraint(hidden, Layout(major_to_minor=(0, 1)))

    rows = full.reshape(x_count, c_count, width // (x_count * c_count), 3 * units)
    sent = down_half(hidden, rows, 1 - core).astype(jnp.bfloat16)
    received = lax.ppermute(sent, "c", [(0, 1), (1, 0)])
    kept = lax.optimization_barrier(down_half(hidden, rows, core))
    paired = (kept + received.astype(jnp.float32)).astype(jnp.bfloat16)
    last_scale, paired = lax.optimization_barrier((down_scale / down_lift, paired))
    parts = lax.all_to_all(paired, "x", 0, 0)
    summed = jnp.sum(parts.astype(jnp.float32), axis=0) * last_scale[:, None]
    return summed.astype(jnp.bfloat16).T


def solution(mesh):
    grid = Mesh(mesh.devices.reshape(16, 4, 4, 2), ("z", "y", "x", "c"))
    fs, tp = ("z", "y"), ("x", "c")
    return jax.shard_map(
        body,
        mesh=grid,
        in_specs=(
            P(fs, None),
            P(),
            P(fs, tp),
            P(fs, tp),
            P(tp),
            P(tp),
            P(None, tp),
            P(None, tp),
            P(tp),
            P(tp),
            P(tp, fs),
            P(tp),
        ),
        out_specs=P(fs, tp),
        check_vma=False,
    )
```

```python
import jax
import jax.numpy as jnp
from jax import lax
from jax.experimental import pallas as pl
from jax.experimental.pallas import tpu as pltpu
from jax.sharding import Mesh, PartitionSpec as P

epsilon = 1e-06
up_lift = 2.0**17
down_lift = 2.0**19
halo = 8
lanes = 128
swap = [(0, 1), (1, 0)]
NT = (((1,), (1,)), ((), ()))


def call(kernel, out_shape, limit, operands, scratch=()):
    vmem = pl.BlockSpec(memory_space=pltpu.VMEM)
    scalar = pl.BlockSpec(memory_space=pltpu.SMEM)
    return pl.pallas_call(
        kernel,
        in_specs=[scalar if o.dtype == jnp.int32 else vmem for o in operands],
        out_specs=vmem,
        out_shape=out_shape,
        scratch_shapes=list(scratch),
        compiler_params=pltpu.CompilerParams(vmem_limit_bytes=limit * 2**20),
    )(*operands)


def hidden_kernel(
    side, tokens, before, near, far, scales, taps, biases, out, ordered
):
    row_count, width = tokens.shape
    units = out.shape[1]
    half = width // 2
    full_rows = ordered.shape[0]
    squares = jnp.zeros((full_rows, lanes), jnp.float32)
    for k in range(half // lanes):
        for at, which in ((0, side[0]), (half, 1 - side[0])):
            source = pl.ds(pl.multiple_of((2 * k + which) * lanes, lanes), lanes)
            block = jnp.concatenate(
                [tokens[:, source], before[:, source]], axis=0
            )
            ordered[:, at + k * lanes : at + (k + 1) * lanes] = block
            values = block.astype(jnp.float32)
            squares = squares + values * values
    mean = jnp.sum(squares, axis=1, keepdims=True) / width
    factor = lax.rsqrt(mean + epsilon) / up_lift

    def mixed(kind, at, size):
        cut = slice(kind * units + at, kind * units + at + size)
        raw = jnp.dot(ordered[:, :half], near[:, cut], preferred_element_type=jnp.float32)
        raw = raw + jnp.dot(ordered[:, half:], far[:, cut], preferred_element_type=jnp.float32)
        pre = (raw * (factor * scales[kind : kind + 1, at : at + size])).astype(jnp.bfloat16)
        pre = pre.astype(jnp.float32)
        total = biases[kind : kind + 1, at : at + size]
        for back_by in range(3):
            shifted = pltpu.roll(pre, back_by, 0) if back_by else pre
            row = 3 * kind + 2 - back_by
            total = total + taps[row : row + 1, at : at + size] * shifted[:row_count]
        return total

    for at in range(0, units, 2 * lanes):
        size = min(2 * lanes, units - at)
        gate = mixed(0, at, size)
        value = mixed(1, at, size)
        out[:, at : at + size] = (jax.nn.gelu(gate, approximate=True) * value).astype(jnp.bfloat16)


def hidden_units(side, tokens, before, near, far, scales, taps, biases):
    row_count, width = tokens.shape
    units = scales.shape[1]
    return call(
        hidden_kernel,
        jax.ShapeDtypeStruct((row_count, units), jnp.bfloat16),
        32,
        (side, tokens, before, near, far, scales, taps, biases),
        [pltpu.VMEM((row_count + before.shape[0], width), jnp.bfloat16)],
    )


def down_kernel(places, hidden, near, far, out, rows):
    side, core = places[0], places[1]
    groups = out.shape[0]
    first = pl.ds(pl.multiple_of(side * lanes, lanes), lanes)
    second = pl.ds(pl.multiple_of((1 - side) * lanes, lanes), lanes)
    for x in range(groups):
        rows[x, first] = near[2 * x + core]
        rows[x, second] = far[2 * x + core]
        product = lax.dot_general(
            hidden[...], rows[x], NT, preferred_element_type=jnp.float32
        )
        out[x] = product.astype(out.dtype)


def down_half(side, core, hidden, near, far, dtype):
    groups = near.shape[0] // 2
    row_count, units = hidden.shape
    return call(
        down_kernel,
        jax.ShapeDtypeStruct((groups, row_count, 2 * lanes), dtype),
        16,
        (jnp.stack([side, core]), hidden, near, far),
        [pltpu.VMEM((groups, 2 * lanes, units), jnp.bfloat16)],
    )


def body(
    tokens,
    norm_gain,
    gate_weight,
    value_weight,
    gate_scale,
    value_scale,
    gate_kernel,
    value_kernel,
    gate_bias,
    value_bias,
    down_weight,
    down_scale,
):
    side, core = lax.axis_index("zl"), lax.axis_index("c")
    place = lax.axis_index(("zh", "zl", "y"))
    count = lax.axis_size(("zh", "zl", "y"))
    row_count, width = tokens.shape
    piece, units = gate_weight.shape

    before = lax.ppermute(
        tokens[row_count - halo :],
        ("zh", "zl", "y"),
        [(source, source + 1) for source in range(count - 1)],
    )
    gain = lax.dynamic_slice(norm_gain, (place * piece,), (piece,))[:, None] * up_lift
    shard = jnp.concatenate(
        [gate_weight * gain, value_weight * gain, down_weight.T * down_lift], axis=1
    ).astype(jnp.float16)
    over_z = lax.all_gather(shard, "zh", axis=0)
    partner = lax.ppermute(over_z[:, :, : 2 * units], "zl", swap)
    near = lax.all_gather(over_z, "y", axis=1, tiled=True)
    near_down = near[:, :, 2 * units :].astype(jnp.bfloat16)
    far_down = lax.ppermute(near_down, "zl", swap)
    far = lax.all_gather(partner, "y", axis=1, tiled=True)
    near_up = near[:, :, : 2 * units].astype(jnp.bfloat16).reshape(width // 2, 2 * units)
    far_up = far.astype(jnp.bfloat16).reshape(width // 2, 2 * units)

    before = jnp.concatenate([jnp.zeros_like(before), before], axis=0)
    hidden = hidden_units(
        side.reshape(1),
        tokens,
        before,
        near_up,
        far_up,
        jnp.stack([gate_scale, value_scale]),
        jnp.concatenate([gate_kernel, value_kernel], axis=0),
        jnp.stack([gate_bias, value_bias]),
    )
    sent = down_half(side, 1 - core, hidden, near_down, far_down, jnp.bfloat16)
    received = lax.ppermute(sent, "c", swap)
    kept = down_half(side, core, hidden, near_down, far_down, jnp.float32)
    paired = (kept + received.astype(jnp.float32)).astype(jnp.bfloat16)
    last_scale, paired = lax.optimization_barrier((down_scale / down_lift, paired))
    parts = lax.all_to_all(paired, "x", 0, 0)
    summed = jnp.sum(parts.astype(jnp.float32), axis=0) * last_scale[None, :]
    return summed.astype(jnp.bfloat16)


def solution(mesh):
    grid = Mesh(mesh.devices.reshape(8, 2, 4, 4, 2), ("zh", "zl", "y", "x", "c"))
    fs, tp = ("zh", "zl", "y"), ("x", "c")
    return jax.shard_map(
        body,
        mesh=grid,
        in_specs=(
            P(fs, None),
            P(),
            P(fs, tp),
            P(fs, tp),
            P(tp),
            P(tp),
            P(None, tp),
            P(None, tp),
            P(tp),
            P(tp),
            P(tp, fs),
            P(tp),
        ),
        out_specs=P(fs, tp),
        check_vma=False,
    )
```

```python
import jax
import jax.numpy as jnp
from jax import lax
from jax.experimental import pallas as pl
from jax.experimental.pallas import tpu as pltpu
from jax.sharding import Mesh, PartitionSpec as P

epsilon = 1e-06
up_lift = 2.0**17
down_lift = 2.0**19
halo = 8
lanes = 128
swap = [(0, 1), (1, 0)]
NT = (((1,), (1,)), ((), ()))


def call(kernel, out_shape, limit, operands, scratch=(), anywhere=()):
    vmem = pl.BlockSpec(memory_space=pltpu.VMEM)
    scalar = pl.BlockSpec(memory_space=pltpu.SMEM)
    remote = pl.BlockSpec(memory_space=pltpu.HBM)
    return pl.pallas_call(
        kernel,
        in_specs=[
            remote if i in anywhere else scalar if o.dtype == jnp.int32 else vmem
            for i, o in enumerate(operands)
        ],
        out_specs=vmem,
        out_shape=out_shape,
        scratch_shapes=list(scratch),
        compiler_params=pltpu.CompilerParams(vmem_limit_bytes=limit * 2**20),
    )(*operands)


def hidden_kernel(
    side, tokens, before, near_source, far, scales, taps, biases, out, ordered, near, arrived
):
    row_count, width = tokens.shape
    units = out.shape[1]
    half = width // 2

    fetch = pltpu.make_async_copy(near_source, near, arrived)
    fetch.start()
    full_rows = ordered.shape[0]
    squares = jnp.zeros((full_rows, lanes), jnp.float32)
    for k in range(half // lanes):
        for at, which in ((0, side[0]), (half, 1 - side[0])):
            source = pl.ds(pl.multiple_of((2 * k + which) * lanes, lanes), lanes)
            block = jnp.concatenate([tokens[:, source], before[:, source]], axis=0)
            ordered[:, at + k * lanes : at + (k + 1) * lanes] = block
            values = block.astype(jnp.float32)
            squares = squares + values * values
    mean = jnp.sum(squares, axis=1, keepdims=True) / width
    factor = lax.rsqrt(mean + epsilon) / up_lift
    fetch.wait()

    for at in range(0, units, lanes):
        gate_cut, value_cut = slice(at, at + lanes), slice(units + at, units + at + lanes)

        def pair(ref):
            return jnp.concatenate([ref[:, gate_cut], ref[:, value_cut]], axis=1)

        raw = jnp.dot(ordered[:, half:], pair(far), preferred_element_type=jnp.float32)
        raw = raw + jnp.dot(ordered[:, :half], pair(near), preferred_element_type=jnp.float32)
        pre = raw * factor
        weights = taps[:, at : at + lanes] * jnp.concatenate(
            [jnp.broadcast_to(scales[kind : kind + 1, at : at + lanes], (3, lanes)) for kind in (0, 1)]
        )
        both = jnp.concatenate([weights[:3], weights[3:]], axis=1)
        total = both[0:1] * pre
        for row in (1, 2):
            total = pltpu.roll(total, 1, 0) + both[row : row + 1] * pre
        gate = total[:row_count, :lanes] + biases[0:1, at : at + lanes]
        value = total[:row_count, lanes:] + biases[1:2, at : at + lanes]
        out[:, at : at + lanes] = (jax.nn.gelu(gate, approximate=True) * value).astype(jnp.bfloat16)


def hidden_units(side, tokens, before, near, far, scales, taps, biases):
    row_count, width = tokens.shape
    units = scales.shape[1]
    return call(
        hidden_kernel,
        jax.ShapeDtypeStruct((row_count, units), jnp.bfloat16),
        32,
        (side, tokens, before, near, far, scales, taps, biases),
        [
            pltpu.VMEM((row_count + before.shape[0], width), jnp.bfloat16),
            pltpu.VMEM(near.shape, near.dtype),
            pltpu.SemaphoreType.DMA,
        ],
        anywhere=(3,),
    )


def down_kernel(places, hidden, near, far, out, rows):
    side, core = places[0], places[1]
    groups = out.shape[0]
    first = pl.ds(pl.multiple_of(side * lanes, lanes), lanes)
    second = pl.ds(pl.multiple_of((1 - side) * lanes, lanes), lanes)
    for x in range(groups):
        rows[x, first] = near[2 * x + core]
        rows[x, second] = far[2 * x + core]
        product = lax.dot_general(
            hidden[...], rows[x], NT, preferred_element_type=jnp.float32
        )
        out[x] = product.astype(out.dtype)


def down_half(side, core, hidden, near, far, dtype):
    groups = near.shape[0] // 2
    row_count, units = hidden.shape
    return call(
        down_kernel,
        jax.ShapeDtypeStruct((groups, row_count, 2 * lanes), dtype),
        16,
        (jnp.stack([side, core]), hidden, near, far),
        [pltpu.VMEM((groups, 2 * lanes, units), jnp.bfloat16)],
    )


def body(
    tokens,
    norm_gain,
    gate_weight,
    value_weight,
    gate_scale,
    value_scale,
    gate_kernel,
    value_kernel,
    gate_bias,
    value_bias,
    down_weight,
    down_scale,
):
    side, core = lax.axis_index("zl"), lax.axis_index("c")
    place = lax.axis_index(("zh", "zl", "y"))
    count = lax.axis_size(("zh", "zl", "y"))
    row_count, width = tokens.shape
    piece, units = gate_weight.shape

    before = lax.ppermute(
        tokens[row_count - halo :],
        ("zh", "zl", "y"),
        [(source, source + 1) for source in range(count - 1)],
    )
    gain = lax.dynamic_slice(norm_gain, (place * piece,), (piece,))[:, None] * up_lift
    shard = jnp.concatenate(
        [gate_weight * gain, value_weight * gain, down_weight.T * down_lift], axis=1
    ).astype(jnp.float16)
    over_z = lax.all_gather(shard, "zh", axis=0)
    partner = lax.ppermute(over_z[:, :, : 2 * units], "zl", swap)
    near = lax.all_gather(over_z, "y", axis=1, tiled=True)
    near_down = near[:, :, 2 * units :].astype(jnp.bfloat16)
    far_down = lax.ppermute(near_down, "zl", swap)
    far = lax.all_gather(partner, "y", axis=1, tiled=True)
    near_up = near[:, :, : 2 * units].astype(jnp.bfloat16).reshape(width // 2, 2 * units)
    far_up = far.astype(jnp.bfloat16).reshape(width // 2, 2 * units)

    before = jnp.concatenate([jnp.zeros_like(before), before], axis=0)
    hidden = hidden_units(
        side.reshape(1),
        tokens,
        before,
        near_up,
        far_up,
        jnp.stack([gate_scale, value_scale]),
        jnp.concatenate([gate_kernel, value_kernel], axis=0),
        jnp.stack([gate_bias, value_bias]),
    )
    sent = down_half(side, 1 - core, hidden, near_down, far_down, jnp.bfloat16)
    received = lax.ppermute(sent, "c", swap)
    kept = down_half(side, core, hidden, near_down, far_down, jnp.float32)
    paired = (kept + received.astype(jnp.float32)).astype(jnp.bfloat16)
    last_scale, paired = lax.optimization_barrier((down_scale / down_lift, paired))
    parts = lax.all_to_all(paired, "x", 0, 0)
    summed = jnp.sum(parts.astype(jnp.float32), axis=0) * last_scale[None, :]
    return summed.astype(jnp.bfloat16)


def solution(mesh):
    grid = Mesh(mesh.devices.reshape(8, 2, 4, 4, 2), ("zh", "zl", "y", "x", "c"))
    fs, tp = ("zh", "zl", "y"), ("x", "c")
    return jax.shard_map(
        body,
        mesh=grid,
        in_specs=(
            P(fs, None),
            P(),
            P(fs, tp),
            P(fs, tp),
            P(tp),
            P(tp),
            P(None, tp),
            P(None, tp),
            P(tp),
            P(tp),
            P(tp, fs),
            P(tp),
        ),
        out_specs=P(fs, tp),
        check_vma=False,
    )
```

```python
import jax
import jax.numpy as jnp
from jax import lax
from jax.experimental import pallas as pl
from jax.experimental.pallas import tpu as pltpu
from jax.sharding import Mesh, PartitionSpec as P

epsilon = 1e-06
up_lift = 2.0**17
down_lift = 2.0**19
halo = 8
lanes = 128
swap = [(0, 1), (1, 0)]
NT = (((1,), (1,)), ((), ()))


def call(kernel, out_shape, limit, operands, scratch=(), anywhere=()):
    vmem = pl.BlockSpec(memory_space=pltpu.VMEM)
    scalar = pl.BlockSpec(memory_space=pltpu.SMEM)
    remote = pl.BlockSpec(memory_space=pltpu.HBM)
    return pl.pallas_call(
        kernel,
        in_specs=[
            remote if i in anywhere else scalar if o.dtype == jnp.int32 else vmem
            for i, o in enumerate(operands)
        ],
        out_specs=vmem,
        out_shape=out_shape,
        scratch_shapes=list(scratch),
        compiler_params=pltpu.CompilerParams(vmem_limit_bytes=limit * 2**20),
    )(*operands)


def hidden_kernel(
    side,
    tokens,
    before,
    near_source,
    far,
    scales,
    taps,
    biases,
    gains,
    out,
    ordered,
    near,
    arrived,
):
    row_count, width = tokens.shape
    units = out.shape[1]
    half = width // 2

    fetch = pltpu.make_async_copy(near_source.at[:, : near.shape[1]], near, arrived)
    fetch.start()
    full_rows = ordered.shape[0]
    squares = jnp.zeros((full_rows, lanes), jnp.float32)
    for k in range(half // lanes):
        for at, which in ((0, side[0]), (half, 1 - side[0])):
            source = pl.ds(pl.multiple_of((2 * k + which) * lanes, lanes), lanes)
            block = jnp.concatenate([tokens[:, source], before[:, source]], axis=0)
            values = block.astype(jnp.float32)
            squares = squares + values * values
            ordered[:, at + k * lanes : at + (k + 1) * lanes] = (
                values * gains[:, source]
            ).astype(jnp.bfloat16)
    mean = jnp.sum(squares, axis=1, keepdims=True) / width
    factor = lax.rsqrt(mean + epsilon) / up_lift
    fetch.wait()

    for at in range(0, units, lanes):
        gate_cut, value_cut = slice(at, at + lanes), slice(units + at, units + at + lanes)

        def pair(ref):
            return jnp.concatenate([ref[:, gate_cut], ref[:, value_cut]], axis=1)

        raw = jnp.dot(ordered[:, half:], pair(far), preferred_element_type=jnp.float32)
        raw = raw + jnp.dot(ordered[:, :half], pair(near), preferred_element_type=jnp.float32)
        pre = raw * factor
        weights = taps[:, at : at + lanes] * jnp.concatenate(
            [jnp.broadcast_to(scales[kind : kind + 1, at : at + lanes], (3, lanes)) for kind in (0, 1)]
        )
        both = jnp.concatenate([weights[:3], weights[3:]], axis=1)
        total = both[0:1] * pre
        for row in (1, 2):
            total = pltpu.roll(total, 1, 0) + both[row : row + 1] * pre
        gate = total[:row_count, :lanes] + biases[0:1, at : at + lanes]
        value = total[:row_count, lanes:] + biases[1:2, at : at + lanes]
        out[:, at : at + lanes] = (jax.nn.gelu(gate, approximate=True) * value).astype(jnp.bfloat16)


def hidden_units(side, tokens, before, near, far, scales, taps, biases, gains):
    row_count, width = tokens.shape
    units = scales.shape[1]
    return call(
        hidden_kernel,
        jax.ShapeDtypeStruct((row_count, units), jnp.bfloat16),
        32,
        (side, tokens, before, near, far, scales, taps, biases, gains),
        [
            pltpu.VMEM((row_count + before.shape[0], width), jnp.bfloat16),
            pltpu.VMEM(far.shape, far.dtype),
            pltpu.SemaphoreType.DMA,
        ],
        anywhere=(3,),
    )


def down_kernel(places, hidden, near, far, out, rows):
    side, core = places[0], places[1]
    groups = out.shape[0]
    first = pl.ds(pl.multiple_of(side * lanes, lanes), lanes)
    second = pl.ds(pl.multiple_of((1 - side) * lanes, lanes), lanes)
    for x in range(groups):
        rows[x, first] = near[2 * x + core, :, near.shape[2] - rows.shape[2] :]
        rows[x, second] = far[2 * x + core]
        product = lax.dot_general(
            hidden[...], rows[x], NT, preferred_element_type=jnp.float32
        )
        out[x] = product.astype(out.dtype)


def down_half(side, core, hidden, near, far, dtype):
    groups = near.shape[0] // 2
    row_count, units = hidden.shape
    return call(
        down_kernel,
        jax.ShapeDtypeStruct((groups, row_count, 2 * lanes), dtype),
        16,
        (jnp.stack([side, core]), hidden, near, far),
        [pltpu.VMEM((groups, 2 * lanes, units), jnp.bfloat16)],
    )


def body(
    tokens,
    norm_gain,
    gate_weight,
    value_weight,
    gate_scale,
    value_scale,
    gate_kernel,
    value_kernel,
    gate_bias,
    value_bias,
    down_weight,
    down_scale,
):
    side, core = lax.axis_index("zl"), lax.axis_index("c")
    count = lax.axis_size(("zh", "zl", "y"))
    row_count, width = tokens.shape
    piece, units = gate_weight.shape

    before = lax.ppermute(
        tokens[row_count - halo :],
        ("zh", "zl", "y"),
        [(source, source + 1) for source in range(count - 1)],
    )
    shard = jnp.concatenate(
        [gate_weight * up_lift, value_weight * up_lift, down_weight.T * down_lift], axis=1
    ).astype(jnp.float16)
    over_z = lax.all_gather(shard, "zh", axis=0)
    partner = lax.ppermute(over_z[:, :, : 2 * units], "zl", swap)
    near = lax.all_gather(over_z, "y", axis=1, tiled=True)
    near = near.astype(jnp.bfloat16)
    far_down = lax.ppermute(near[:, :, 2 * units :], "zl", swap)
    far = lax.all_gather(partner, "y", axis=1, tiled=True)
    near_up = near.reshape(width // 2, 3 * units)
    far_up = far.astype(jnp.bfloat16).reshape(width // 2, 2 * units)

    before = jnp.concatenate([jnp.zeros_like(before), before], axis=0)
    hidden = hidden_units(
        side.reshape(1),
        tokens,
        before,
        near_up,
        far_up,
        jnp.stack([gate_scale, value_scale]),
        jnp.concatenate([gate_kernel, value_kernel], axis=0),
        jnp.stack([gate_bias, value_bias]),
        norm_gain[None, :],
    )
    sent = down_half(side, 1 - core, hidden, near, far_down, jnp.bfloat16)
    received = lax.ppermute(sent, "c", swap)
    kept = down_half(side, core, hidden, near, far_down, jnp.float32)
    paired = (kept + received.astype(jnp.float32)).astype(jnp.bfloat16)
    last_scale, paired = lax.optimization_barrier((down_scale / down_lift, paired))
    parts = lax.all_to_all(paired, "x", 0, 0)
    summed = jnp.sum(parts.astype(jnp.float32), axis=0) * last_scale[None, :]
    return summed.astype(jnp.bfloat16)


def solution(mesh):
    grid = Mesh(mesh.devices.reshape(8, 2, 4, 4, 2), ("zh", "zl", "y", "x", "c"))
    fs, tp = ("zh", "zl", "y"), ("x", "c")
    return jax.shard_map(
        body,
        mesh=grid,
        in_specs=(
            P(fs, None),
            P(),
            P(fs, tp),
            P(fs, tp),
            P(tp),
            P(tp),
            P(None, tp),
            P(None, tp),
            P(tp),
            P(tp),
            P(tp, fs),
            P(tp),
        ),
        out_specs=P(fs, tp),
        check_vma=False,
    )
```

```python
import jax
import jax.numpy as jnp
from jax import lax
from jax.experimental import pallas as pl
from jax.experimental.pallas import tpu as pltpu
from jax.sharding import Mesh, PartitionSpec as P

epsilon = 1e-06
up_lift = 2.0**17
down_lift = 2.0**19
halo = 8
lanes = 128
swap = [(0, 1), (1, 0)]
NT = (((1,), (1,)), ((), ()))


def call(kernel, out_shape, limit, operands, scratch=(), anywhere=()):
    vmem = pl.BlockSpec(memory_space=pltpu.VMEM)
    scalar = pl.BlockSpec(memory_space=pltpu.SMEM)
    remote = pl.BlockSpec(memory_space=pltpu.HBM)
    return pl.pallas_call(
        kernel,
        in_specs=[
            remote if i in anywhere else scalar if o.dtype == jnp.int32 else vmem
            for i, o in enumerate(operands)
        ],
        out_specs=vmem,
        out_shape=out_shape,
        scratch_shapes=list(scratch),
        compiler_params=pltpu.CompilerParams(vmem_limit_bytes=limit * 2**20),
    )(*operands)


def hidden_kernel(
    side,
    tokens,
    before,
    near,
    far,
    scales,
    taps,
    biases,
    gains,
    out,
    ordered,
):
    row_count, width = tokens.shape
    units = out.shape[1]
    half = width // 2

    full_rows = ordered.shape[0]
    squares = jnp.zeros((full_rows, lanes), jnp.float32)
    for k in range(half // lanes):
        for at, which in ((0, side[0]), (half, 1 - side[0])):
            source = pl.ds(pl.multiple_of((2 * k + which) * lanes, lanes), lanes)
            block = jnp.concatenate([tokens[:, source], before[:, source]], axis=0)
            values = block.astype(jnp.float32)
            squares = squares + values * values
            ordered[:, at + k * lanes : at + (k + 1) * lanes] = (
                values * gains[:, source]
            ).astype(jnp.bfloat16)
    mean = jnp.sum(squares, axis=1, keepdims=True) / width
    factor = lax.rsqrt(mean + epsilon) / up_lift

    for at in range(0, units, lanes):
        gate_cut, value_cut = slice(at, at + lanes), slice(units + at, units + at + lanes)

        def pair(ref):
            return jnp.concatenate([ref[:, gate_cut], ref[:, value_cut]], axis=1)

        raw = jnp.dot(ordered[:, half:], pair(far), preferred_element_type=jnp.float32)
        raw = raw + jnp.dot(ordered[:, :half], pair(near), preferred_element_type=jnp.float32)
        pre = raw * factor
        weights = taps[:, at : at + lanes] * jnp.concatenate(
            [jnp.broadcast_to(scales[kind : kind + 1, at : at + lanes], (3, lanes)) for kind in (0, 1)]
        )
        both = jnp.concatenate([weights[:3], weights[3:]], axis=1)
        total = both[0:1] * pre
        for row in (1, 2):
            total = pltpu.roll(total, 1, 0) + both[row : row + 1] * pre
        gate = total[:row_count, :lanes] + biases[0:1, at : at + lanes]
        value = total[:row_count, lanes:] + biases[1:2, at : at + lanes]
        out[:, at : at + lanes] = (jax.nn.gelu(gate, approximate=True) * value).astype(jnp.bfloat16)


def hidden_units(side, tokens, before, near, far, scales, taps, biases, gains):
    row_count, width = tokens.shape
    units = scales.shape[1]
    return call(
        hidden_kernel,
        jax.ShapeDtypeStruct((row_count, units), jnp.bfloat16),
        32,
        (side, tokens, before, near, far, scales, taps, biases, gains),
        [
            pltpu.VMEM((row_count + before.shape[0], width), jnp.bfloat16),
        ],
    )


def down_kernel(places, hidden, near, far, out, rows):
    side, core = places[0], places[1]
    groups = out.shape[0]
    first = pl.ds(pl.multiple_of(side * lanes, lanes), lanes)
    second = pl.ds(pl.multiple_of((1 - side) * lanes, lanes), lanes)
    for x in range(groups):
        rows[x, first] = near[2 * x + core, :, near.shape[2] - rows.shape[2] :]
        rows[x, second] = far[2 * x + core]
        product = lax.dot_general(
            hidden[...], rows[x], NT, preferred_element_type=jnp.float32
        )
        out[x] = product.astype(out.dtype)


def down_half(side, core, hidden, near, far, dtype):
    groups = near.shape[0] // 2
    row_count, units = hidden.shape
    return call(
        down_kernel,
        jax.ShapeDtypeStruct((groups, row_count, 2 * lanes), dtype),
        16,
        (jnp.stack([side, core]), hidden, near, far),
        [pltpu.VMEM((groups, 2 * lanes, units), jnp.bfloat16)],
    )


def final_kernel(parts, scale, out):
    summed = parts[0].astype(jnp.float32)
    for x in range(1, parts.shape[0]):
        summed = summed + parts[x].astype(jnp.float32)
    out[...] = (summed * scale[...]).astype(jnp.bfloat16)


def body(
    tokens,
    norm_gain,
    gate_weight,
    value_weight,
    gate_scale,
    value_scale,
    gate_kernel,
    value_kernel,
    gate_bias,
    value_bias,
    down_weight,
    down_scale,
):
    side, core = lax.axis_index("zl"), lax.axis_index("c")
    count = lax.axis_size(("zh", "zl", "y"))
    row_count, width = tokens.shape
    piece, units = gate_weight.shape

    before = lax.ppermute(
        tokens[row_count - halo :],
        ("zh", "zl", "y"),
        [(source, source + 1) for source in range(count - 1)],
    )
    shard = jnp.concatenate(
        [gate_weight * up_lift, value_weight * up_lift, down_weight.T * down_lift], axis=1
    ).astype(jnp.float16)
    over_z = lax.all_gather(shard, "zh", axis=0)
    partner = lax.ppermute(over_z[:, :, : 2 * units], "zl", swap)
    near = lax.all_gather(over_z, "y", axis=1, tiled=True)
    near = near.astype(jnp.bfloat16)
    far_down = lax.ppermute(near[:, :, 2 * units :], "zl", swap)
    far = lax.all_gather(partner, "y", axis=1, tiled=True)
    near_up = near.reshape(width // 2, 3 * units)
    far_up = far.astype(jnp.bfloat16).reshape(width // 2, 2 * units)

    before = jnp.concatenate([jnp.zeros_like(before), before], axis=0)
    hidden = hidden_units(
        side.reshape(1),
        tokens,
        before,
        near_up,
        far_up,
        jnp.stack([gate_scale, value_scale]),
        jnp.concatenate([gate_kernel, value_kernel], axis=0),
        jnp.stack([gate_bias, value_bias]),
        norm_gain[None, :],
    )
    sent = down_half(side, 1 - core, hidden, near, far_down, jnp.bfloat16)
    received = lax.ppermute(sent, "c", swap)
    kept = down_half(side, core, hidden, near, far_down, jnp.float32)
    paired = (kept + received.astype(jnp.float32)).astype(jnp.bfloat16)
    last_scale, paired = lax.optimization_barrier((down_scale / down_lift, paired))
    parts = lax.all_to_all(paired, "x", 0, 0)
    return call(
        final_kernel,
        jax.ShapeDtypeStruct(parts.shape[1:], jnp.bfloat16),
        8,
        (parts, last_scale[None, :]),
    )


def solution(mesh):
    grid = Mesh(mesh.devices.reshape(8, 2, 4, 4, 2), ("zh", "zl", "y", "x", "c"))
    fs, tp = ("zh", "zl", "y"), ("x", "c")
    return jax.shard_map(
        body,
        mesh=grid,
        in_specs=(
            P(fs, None),
            P(),
            P(fs, tp),
            P(fs, tp),
            P(tp),
            P(tp),
            P(None, tp),
            P(None, tp),
            P(tp),
            P(tp),
            P(tp, fs),
            P(tp),
        ),
        out_specs=P(fs, tp),
        check_vma=False,
    )
```
